32 devices in a mesh: sp: 4 (over y, x), tp: 8 (over z, core).
Axes of the slice: x: 2, y: 2, z: 4, core: 2. Of those that a mesh axis runs over, the one named last changes fastest.
Arguments:
- residual: bfloat16 [1536, 2048], P(('sp', 'tp')), may hold values from -40 to 40
- queries: bfloat16 [1536, 16, 256], P('sp', 'tp'), may hold values from -8.8 to 8.8
- query_rope: bfloat16 [1536, 16, 64], P('sp', 'tp'), may hold values from -72 to 72
- latent: bfloat16 [1536, 512], P('sp'), may hold values from -320 to 320
- key_rope: bfloat16 [1536, 32], P('sp'), may hold values from -48 to 48
- latent_gain: float32 [512], replicated, may hold values from 0.1 to 1.9
- key_weight: bfloat16 [512, 16, 256], P(None, 'tp'), may hold values from -0.25 to 0.25
- value_weight: bfloat16 [512, 16, 256], P(None, 'tp'), may hold values from -0.25 to 0.25
- out_weight: bfloat16 [16, 256, 2048], P('tp'), may hold values from -0.09375 to 0.09375
- norm_gain: float32 [2048], replicated, may hold values from 0.1 to 1.9
- routes: int32 [1536, 2], P('sp'), may hold values from 0 to 7, as said below
- group_gate: float32 [1536], P(('sp', 'tp')), may hold values from 0.5 to 1
- expert_share: float32 [1536, 2], P(('sp', 'tp')), may hold values from 0.2 to 1
- gate_weight: bfloat16 [8, 2048, 4096], P('sp', None, 'tp'), may hold values from -0.125 to 0.125
- up_weight: bfloat16 [8, 2048, 4096], P('sp', None, 'tp'), may hold values from -0.125 to 0.125
- down_weight: bfloat16 [8, 4096, 2048], P('sp', 'tp'), may hold values from -0.1875 to 0.1875
Outputs:
- layer_out: bfloat16 [1536, 2048], P(('sp', 'tp'))
The draws below stay inside these ranges and needn't reach their ends.
Inputs may be any that keep to these rules, and one draw needn't show every extreme that they name: `routes`: each token names two different experts of one group; expert e belongs to group e // 2. In each aligned block of 48 tokens no expert is named more than 18 times, and one expert, the same in every block, is named exactly 18 times in every block.
All inputs are finite; a program needn't handle non-finite values.
Results may differ from the reference program's by a relative error of at most 0.025.
Values may be sent and summed in bfloat16 or wider, within the bound.
A program may use at most 64 MiB of HBM per device.

```python
import math
import jax
import jax.numpy as jnp
from jax import lax

D = 2048
PAIRS = 16
DK_A = 64
DV_A = 64
DK_B = 192
DV_B = 192
DR = 32
LATENT = 512
FF = 4096
GROUPS = 4
TOPK = 2
SEQ = 1536
PAIR_DEV = 2
ROWS = 48
FF_DEV = 512
EXPERTS = 8
CAP = 18
N_TP = 8


def rough_field(key, salt_value, columns):
    values = jnp.clip(jax.random.normal(jax.random.fold_in(key, salt_value), (SEQ, columns), jnp.float32), -4.0, 4.0)
    return values


def draw_residual(key, part):
    return (0.25 * rough_field(key, 40, D)).astype(jnp.bfloat16)


def draw_latent(key, part):
    return rough_field(key, 50, LATENT).astype(jnp.bfloat16)


def draw_queries(key, part):
    own_key = jax.random.fold_in(key, 23)
    array_shape = (SEQ, PAIRS, DK_A + DK_B)
    return jnp.clip(2.2 * jax.random.normal(own_key, array_shape, jnp.float32), -8.75, 8.75).astype(jnp.bfloat16)


def draw_query_rope(key, part):
    own_key = jax.random.fold_in(key, 21)
    array_shape = (SEQ, PAIRS, 2 * DR)
    return jnp.clip(2.2 * jax.random.normal(own_key, array_shape, jnp.float32), -8.75, 8.75).astype(jnp.bfloat16)


def draw_key_rope(key, part):
    own_key = jax.random.fold_in(key, 22)
    base_values = jnp.clip(jax.random.normal(own_key, (SEQ, DR), jnp.float32), -4.0, 4.0)
    return base_values.astype(jnp.bfloat16)


def draw_routes(key, part):
    blocks = SEQ // ROWS
    within = EXPERTS // GROUPS
    pair_total = EXPERTS // 2
    hot_rows = 0
    while hot_rows + (ROWS - hot_rows + pair_total - 1) // pair_total != CAP:
        hot_rows += 1
    key_list = jax.random.split(jax.random.fold_in(key, 31), 5)
    favored = jax.random.randint(key_list[0], (), 0, EXPERTS, dtype=jnp.int32)
    favored_group = favored // within
    favored_place = favored % within
    member = jnp.arange(within, dtype=jnp.int32)
    ranking = jax.random.randint(key_list[1], (blocks, GROUPS, within), 0, 1 << 20, dtype=jnp.int32) * within + member
    place_order = jnp.argsort(ranking, axis=2).astype(jnp.int32)
    leading = place_order[:, :, :1]
    swapped = jnp.where(place_order == favored_place, leading, place_order)
    swapped = jnp.where(member[None, None, :] == 0, favored_place, swapped)
    is_favored = (jnp.arange(GROUPS, dtype=jnp.int32) == favored_group)[None, :, None]
    place_order = jnp.where(is_favored, swapped, place_order)
    expert_table = place_order + (jnp.arange(GROUPS, dtype=jnp.int32) * within)[None, :, None]
    pair_table = expert_table.reshape(blocks, pair_total, 2)
    pair_ids = jnp.arange(pair_total, dtype=jnp.int32)
    pair_rank = jax.random.randint(key_list[2], (blocks, pair_total), 0, 1 << 20, dtype=jnp.int32) * pair_total + pair_ids
    pair_rank = jnp.where(pair_ids[None, :] == favored_group * (within // 2), -1, pair_rank)
    pair_order = jnp.argsort(pair_rank, axis=1)
    pair_table = jnp.take_along_axis(pair_table, pair_order[:, :, None], axis=1)
    row_ids = jnp.arange(ROWS, dtype=jnp.int32)
    cycled = jnp.take(pair_table, (row_ids - hot_rows) % pair_total, axis=1)
    favored_row = jnp.take(expert_table, favored_group, axis=1)
    partner = jnp.take(favored_row, 1 + row_ids % (within - 1), axis=1)
    hot_pair = jnp.stack([jnp.broadcast_to(favored, partner.shape), partner], axis=2)
    chosen = jnp.where((row_ids < hot_rows)[None, :, None], hot_pair, cycled)
    flip_bits = jax.random.randint(key_list[3], (blocks, ROWS, 1), 0, 2, dtype=jnp.int32)
    chosen = jnp.where(flip_bits == 1, chosen[:, :, ::-1], chosen)
    shuffle = jnp.argsort(jax.random.randint(key_list[4], (blocks, ROWS), 0, 1 << 20, dtype=jnp.int32) * ROWS + row_ids[None, :], axis=1)
    chosen = jnp.take_along_axis(chosen, shuffle[:, :, None], axis=1)
    return chosen.reshape(SEQ, 2).astype(jnp.int32)


def block_levels(rng, shape, pieces, smallest, top_value):
    def one(axis_at, parts):
        steps = jax.random.uniform(jax.random.fold_in(jax.random.fold_in(rng, 6), axis_at), (parts,), jnp.float32, smallest / len(pieces), top_value / len(pieces))
        return jnp.repeat(jnp.exp(steps), shape[axis_at] // parts).reshape((-1,) + (1,) * (len(shape) - axis_at - 1))

    level = one(*pieces[0])
    for cut in pieces[1:]:
        level = level * one(*cut)
    return level


def scatter_about(key, shape, deviation, limit, cuts=(), kind=jnp.bfloat16):
    array = jax.random.normal(key, shape, jnp.float32) * deviation
    if len(cuts) > 0:
        array = block_levels(key, shape, cuts, -0.22, 0.18) * array
    return jnp.clip(array, min=-limit, max=limit).astype(kind)


def setup_inputs(seed: int = 0) -> dict:
    splits = jax.random.split(jax.random.key(seed), 17)
    residual = draw_residual(jax.random.fold_in(splits[16], 71), 0)
    queries = draw_queries(jax.random.fold_in(splits[16], 71), 0)
    query_rope = draw_query_rope(jax.random.fold_in(splits[16], 71), 0)
    latent = draw_latent(jax.random.fold_in(splits[16], 71), 0)
    key_rope = draw_key_rope(jax.random.fold_in(splits[16], 71), 0)
    latent_gain = jnp.clip(1.0 + 0.18 * jax.random.normal(splits[5], (LATENT,), jnp.float32), 0.1, 1.9)
    key_weight = scatter_about(splits[6], (LATENT, PAIRS, DK_A + DK_B), LATENT ** -0.5, 0.25, ((1, 8),))
    value_weight = scatter_about(splits[7], (LATENT, PAIRS, DV_A + DV_B), LATENT ** -0.5, 0.25, ((1, 8),))
    out_weight = scatter_about(splits[8], (PAIRS, DV_A + DV_B, D), (PAIRS * (DV_A + DV_B)) ** -0.5, 0.09375, ((0, 8),))
    norm_gain = jnp.clip(1.0 + 0.18 * jax.random.normal(splits[9], (D,), jnp.float32), 0.1, 1.9)
    routes = draw_routes(jax.random.fold_in(splits[16], 71), 0)
    group_gate = jnp.clip(jnp.exp(math.log(1.0) - 0.6931472 * jax.random.uniform(splits[11], (SEQ,), jnp.float32) ** block_levels(splits[11], (SEQ,), ((0, 32),), -0.2, 0.2)), 0.5, 1.0)
    expert_share = jnp.clip(jnp.exp(math.log(1.0) - 1.609438 * jax.random.uniform(splits[12], (SEQ, TOPK), jnp.float32) ** block_levels(splits[12], (SEQ, TOPK), ((0, 32),), -0.2, 0.2)), 0.2, 1.0)
    gate_weight = scatter_about(splits[13], (EXPERTS, D, FF), D ** -0.5, 0.125, ((0, 4), (2, 8)))
    up_weight = scatter_about(splits[14], (EXPERTS, D, FF), D ** -0.5, 0.125, ((0, 4), (2, 8)))
    down_weight = scatter_about(splits[15], (EXPERTS, FF, D), (FF // 4) ** -0.5, 0.1875, ((0, 4), (1, 8)))
    return {"residual": residual, "queries": queries, "query_rope": query_rope, "latent": latent, "key_rope": key_rope, "latent_gain": latent_gain, "key_weight": key_weight, "value_weight": value_weight, "out_weight": out_weight, "norm_gain": norm_gain, "routes": routes, "group_gate": group_gate, "expert_share": expert_share, "gate_weight": gate_weight, "up_weight": up_weight, "down_weight": down_weight}


rope_base = 10000.0
epsilon = 1e-06

def angle_tables(places, rope_width):
    frequencies = rope_base ** (-jnp.arange(0, rope_width, 2, dtype=jnp.float32) / rope_width)
    angles = places[:, None] * frequencies[None, :]
    return (jnp.cos(angles), jnp.sin(angles))

def rope_turn(values, cosine, sine_table):
    half_size = values.shape[-1] // 2
    first_half = values[..., :half_size]
    second = values[..., half_size:]
    return jnp.concatenate([first_half * cosine - second * sine_table, second * cosine + first_half * sine_table], axis=-1)

def rms_scale(values, gain_vector):
    values = values.astype(jnp.float32)
    inverse = lax.rsqrt(lax.optimization_barrier(jnp.mean(values * values, axis=-1, keepdims=True)) + epsilon)
    return values * inverse * gain_vector.astype(jnp.float32)

def group_attend(query_nope, query_turned, key_nope, rotated_key, value_part, visible, scale):
    scores = jnp.einsum('qhd,khd->hqk', query_nope.astype(jnp.float32), key_nope.astype(jnp.float32))
    scores = scores + jnp.einsum('qhd,kd->hqk', query_turned.astype(jnp.float32), rotated_key.astype(jnp.float32))
    scores = scores * scale
    masked = jnp.where(visible[None], scores, -jnp.inf)
    row_top = lax.optimization_barrier(jnp.max(masked, axis=2, keepdims=True))
    weights = jnp.exp(masked - row_top)
    weight_sum = lax.optimization_barrier(jnp.sum(weights, axis=2))
    rounded = lax.optimization_barrier(weights.astype(jnp.bfloat16)).astype(jnp.float32)
    mixed_rows = jnp.einsum('hqk,khd->qhd', rounded, value_part.astype(jnp.float32))
    return (mixed_rows / jnp.transpose(weight_sum)[:, :, None]).astype(jnp.bfloat16)

def reference(residual, queries, query_rope, latent, key_rope, latent_gain, key_weight, value_weight, out_weight, norm_gain, routes, group_gate, expert_share, gate_weight, up_weight, down_weight):
    places = jnp.arange(SEQ, dtype=jnp.int32).astype(jnp.float32)
    cosine, sine_table = angle_tables(places, DR)
    compressed = rms_scale(latent, latent_gain).astype(jnp.bfloat16)
    rotated_key = rope_turn(key_rope.astype(jnp.float32), cosine, sine_table).astype(jnp.bfloat16)
    turned = rope_turn(query_rope.astype(jnp.float32).reshape(SEQ, PAIRS, 2, DR), cosine[:, None, None, :], sine_table[:, None, None, :]).astype(jnp.bfloat16)
    key_rows = jnp.dot(compressed, key_weight.reshape(LATENT, -1), preferred_element_type=jnp.float32).astype(jnp.bfloat16).reshape(SEQ, PAIRS, DK_A + DK_B)
    value_rows = jnp.dot(compressed, value_weight.reshape(LATENT, -1), preferred_element_type=jnp.float32).astype(jnp.bfloat16).reshape(SEQ, PAIRS, DV_A + DV_B)
    scale_one = (DK_A + DR) ** (-0.5)
    scale_two = (DK_B + DR) ** (-0.5)
    block_size = 256

    def attend_block(block_index):
        block_start = block_index * block_size
        query_block = lax.dynamic_slice_in_dim(queries, block_start, block_size, 0)
        turned_block = lax.dynamic_slice_in_dim(turned, block_start, block_size, 0)
        query_places = (block_start + jnp.arange(block_size, dtype=jnp.int32)).astype(jnp.float32)
        visible = query_places[:, None] >= places[None, :]
        part_one = group_attend(query_block[:, :, :DK_A], turned_block[:, :, 0], key_rows[:, :, :DK_A], rotated_key, value_rows[:, :, :DV_A], visible, scale_one)
        part_two = group_attend(query_block[:, :, DK_A:], turned_block[:, :, 1], key_rows[:, :, DK_A:], rotated_key, value_rows[:, :, DV_A:], visible, scale_two)
        return jnp.concatenate([part_one, part_two], axis=2)
    attention = lax.map(attend_block, jnp.arange(SEQ // block_size, dtype=jnp.int32)).reshape(SEQ, PAIRS * (DV_A + DV_B))
    out_flat = out_weight.reshape(PAIRS * (DV_A + DV_B), D)
    run_width = PAIR_DEV * (DV_A + DV_B)

    def add_run(running, run_index):
        columns = lax.dynamic_slice_in_dim(attention, run_index * run_width, run_width, 1)
        weight_rows = lax.dynamic_slice_in_dim(out_flat, run_index * run_width, run_width, 0)
        partial_sum = jnp.dot(columns, weight_rows, preferred_element_type=jnp.float32)
        return (running + lax.optimization_barrier(partial_sum.astype(jnp.bfloat16)).astype(jnp.float32), None)
    head_total, unused = lax.scan(add_run, jnp.zeros((SEQ, D), jnp.float32), jnp.arange(N_TP, dtype=jnp.int32))
    mixed_rows = residual.astype(jnp.float32) + head_total
    normed = rms_scale(mixed_rows, norm_gain).astype(jnp.bfloat16)
    blocks = SEQ // ROWS
    flat_routes = routes.reshape(blocks, ROWS * TOPK)
    onehot = (flat_routes[:, :, None] == jnp.arange(EXPERTS, dtype=jnp.int32)[None, None, :]).astype(jnp.int32)
    rank_within = lax.optimization_barrier(jnp.sum((jnp.cumsum(onehot, axis=1) - onehot) * onehot, axis=2))
    slot_columns = (jnp.arange(blocks, dtype=jnp.int32)[:, None] * CAP + rank_within).reshape(-1).astype(jnp.int32)
    expert_flat = flat_routes.reshape(-1).astype(jnp.int32)
    token_flat = jnp.repeat(jnp.arange(SEQ, dtype=jnp.int32), TOPK)
    token_of = jnp.full((EXPERTS, blocks * CAP), SEQ, dtype=jnp.int32).at[expert_flat, slot_columns].set(token_flat)
    padded = jnp.concatenate([normed, jnp.zeros((1, D), jnp.bfloat16)], axis=0)
    expert_rows = padded[token_of]

    def expert_apply(inputs):
        rows_in, gate_part, up_part, down_part = inputs
        gate_out = jnp.dot(rows_in, gate_part, preferred_element_type=jnp.float32)
        up_out = jnp.dot(rows_in, up_part, preferred_element_type=jnp.float32)
        hidden = (jax.nn.silu(gate_out) * up_out).astype(jnp.bfloat16)
        hidden_runs = hidden.reshape(hidden.shape[0], N_TP, FF_DEV).astype(jnp.float32)
        down_runs = down_part.reshape(N_TP, FF_DEV, D).astype(jnp.float32)
        partial_sum = jnp.einsum('snf,nfd->snd', hidden_runs, down_runs)
        rounded = lax.optimization_barrier(partial_sum.astype(jnp.bfloat16)).astype(jnp.float32)
        return lax.optimization_barrier(jnp.sum(rounded, axis=1)).astype(jnp.bfloat16)
    outputs = lax.map(expert_apply, (expert_rows, gate_weight, up_weight, down_weight))
    picked = outputs[expert_flat, slot_columns].astype(jnp.float32).reshape(SEQ, TOPK, D)
    share_values = expert_share.astype(jnp.float32)
    route_weight = group_gate.astype(jnp.float32)[:, None] * share_values / lax.optimization_barrier(jnp.sum(share_values, axis=1, keepdims=True))
    expert_mix = lax.optimization_barrier(jnp.sum(route_weight[:, :, None] * picked, axis=1))
    return (mixed_rows + expert_mix).astype(jnp.bfloat16)
```

```python
import functools

import jax
import jax.numpy as jnp
from jax import lax
from jax.experimental import pallas as pl
from jax.experimental.pallas import tpu as pltpu
from jax.sharding import PartitionSpec as P

DK_A = 64
DV_A = 64
GROUPS = 4

rope_base = 10000.0
epsilon = 1e-06
floor_score = -1e30
MESH = pl.DeviceIdType.MESH
VM = pl.BlockSpec(memory_space=pltpu.VMEM)


def angle_tables(places, rope_width):
    frequencies = rope_base ** (-jnp.arange(0, rope_width, 2, dtype=jnp.float32) / rope_width)
    angles = places[:, None] * frequencies[None, :]
    return (jnp.cos(angles), jnp.sin(angles))


def rms_scale(values, gain_vector):
    values = values.astype(jnp.float32)
    inverse = lax.rsqrt(jnp.mean(values * values, axis=-1, keepdims=True) + epsilon)
    return values * inverse * gain_vector


def greet(targets):
    barrier = pltpu.get_barrier_semaphore()
    for target in targets:
        pl.semaphore_signal(barrier, inc=1, device_id=target, device_id_type=MESH)
    pl.semaphore_wait(barrier, len(targets))


def remote(src, dst, send, recv, target):
    return pltpu.make_async_remote_copy(
        src_ref=src,
        dst_ref=dst,
        send_sem=send,
        recv_sem=recv,
        device_id=target,
        device_id_type=MESH,
    )


def comm_call(kernel, out_shape, scratch, identity, args):
    return pl.pallas_call(
        kernel,
        out_shape=out_shape,
        in_specs=[VM] * len(args),
        out_specs=VM,
        scratch_shapes=scratch,
        compiler_params=pltpu.CompilerParams(
            collective_id=identity, has_side_effects=True, vmem_limit_bytes=48 * 1024 * 1024
        ),
    )(*args)


def gather_sp_kernel(sp_count, x_ref, out_ref, send, recv, fsend, local_sem):
    me = lax.axis_index("sp")
    tp = lax.axis_index("tp")
    core = lax.rem(tp, 2)
    partner = tp + 1 - 2 * core
    half = x_ref.shape[0] // 2
    greet([(lax.rem(me + k, sp_count), tp) for k in range(1, sp_count)] + [(me, partner)])
    mine = pl.ds(pl.multiple_of(core * half, half), half)
    other = pl.ds(pl.multiple_of((1 - core) * half, half), half)
    own = pltpu.make_async_copy(x_ref, out_ref.at[me], local_sem)
    own.start()

    def outgoing(to):
        return remote(
            x_ref.at[mine], out_ref.at[me, mine], send.at[to], recv.at[me, core], (to, tp)
        )

    def incoming(source):
        return remote(
            x_ref.at[mine],
            out_ref.at[source, mine],
            send.at[source],
            recv.at[source, core],
            (source, tp),
        )

    def forward(source):
        return remote(
            out_ref.at[source, mine],
            out_ref.at[source, mine],
            fsend.at[source],
            recv.at[source, core],
            (me, partner),
        )

    def forwarded(source):
        return remote(
            out_ref.at[source, other],
            out_ref.at[source, other],
            fsend.at[source],
            recv.at[source, 1 - core],
            (me, partner),
        )

    for to in reversed(range(sp_count)):

        @pl.when(to > me)
        def _():
            outgoing(to).start()

    for source in reversed(range(sp_count)):

        @pl.when(source < me)
        def _():
            incoming(source).wait_recv()
            forward(source).start()

    own.wait()
    for source in range(sp_count):

        @pl.when(source < me)
        def _():
            forwarded(source).wait_recv()
            forward(source).wait_send()

        @pl.when(source > me)
        def _():
            outgoing(source).wait_send()


def gather_sp(x, sp_count, identity):
    return comm_call(
        functools.partial(gather_sp_kernel, sp_count),
        jax.ShapeDtypeStruct((sp_count,) + x.shape, x.dtype),
        [
            pltpu.SemaphoreType.DMA((sp_count,)),
            pltpu.SemaphoreType.DMA((sp_count, 2)),
            pltpu.SemaphoreType.DMA((sp_count,)),
            pltpu.SemaphoreType.DMA,
        ],
        identity,
        (x,),
    )


def gather_tp_kernel(tp_count, x_ref, out_ref, send, psend, recv, local_sem):
    sp = lax.axis_index("sp")
    tp = lax.axis_index("tp")
    core = lax.rem(tp, 2)
    z = lax.div(tp, 2)
    depth = tp_count // 2
    partner = tp + 1 - 2 * core
    peers = [lax.rem(z + k, depth) * 2 + core for k in range(1, depth)]
    order = sorted(range(depth - 1), key=lambda i: -min(i + 1, depth - 1 - i))
    greet([(sp, partner)] + [(sp, peer) for peer in peers])
    own = pltpu.make_async_copy(x_ref, out_ref.at[tp], local_sem)
    own.start()
    sends = []
    for i in order:
        copy = remote(x_ref, out_ref.at[tp], send.at[i], recv.at[tp], (sp, peers[i]))
        copy.start()
        sends.append(copy)
    copy = remote(x_ref, out_ref.at[tp], psend.at[depth - 1], recv.at[tp], (sp, partner))
    copy.start()
    sends.append(copy)
    for i in reversed(order):
        block = peers[i]
        remote(x_ref, out_ref.at[block], send.at[i], recv.at[block], (sp, block)).wait_recv()
        copy = remote(
            out_ref.at[block], out_ref.at[block], psend.at[i], recv.at[block], (sp, partner)
        )
        copy.start()
        sends.append(copy)
    for k in range(depth):
        block = lax.rem(z + k, depth) * 2 + 1 - core
        remote(x_ref, out_ref.at[block], psend.at[0], recv.at[block], (sp, partner)).wait_recv()
    for copy in sends:
        copy.wait_send()
    own.wait()


def gather_tp(x, tp_count, identity):
    return comm_call(
        functools.partial(gather_tp_kernel, tp_count),
        jax.ShapeDtypeStruct((tp_count,) + x.shape, x.dtype),
        [
            pltpu.SemaphoreType.DMA((tp_count,)),
            pltpu.SemaphoreType.DMA((tp_count,)),
            pltpu.SemaphoreType.DMA((tp_count,)),
            pltpu.SemaphoreType.DMA,
        ],
        identity,
        (x,),
    )


def reduce_tp_kernel(
    tp_count, x_ref, out_ref, partner_in, stage, z_in, send, recv, zsend, zrecv
):
    sp = lax.axis_index("sp")
    tp = lax.axis_index("tp")
    core = lax.rem(tp, 2)
    z = lax.div(tp, 2)
    depth = tp_count // 2
    partner = tp + 1 - 2 * core
    offsets = sorted(range(1, depth), key=lambda k: -min(k, depth - k)) + [0]
    places = [lax.rem(z + k, depth) for k in offsets]
    greet([(sp, partner)] + [(sp, place * 2 + core) for place in places[:-1]])
    swaps = []
    for place in places:
        copy = remote(
            x_ref.at[place * 2 + 1 - core],
            partner_in.at[place],
            send.at[place],
            recv.at[place],
            (sp, partner),
        )
        copy.start()
        swaps.append(copy)
    sends = []
    total = None
    for i, place in enumerate(places):
        swaps[i].wait_recv()
        total = x_ref[place * 2 + core].astype(jnp.float32) + partner_in[place].astype(jnp.float32)
        if i < depth - 1:
            stage[place] = total.astype(stage.dtype)
        else:
            out_ref[...] = total
        if i > 0:
            back = places[i - 1]
            copy = remote(
                stage.at[back], z_in.at[z], zsend.at[back], zrecv.at[z], (sp, back * 2 + core)
            )
            copy.start()
            sends.append(copy)
    for place in reversed(places[:-1]):
        remote(
            stage.at[place], z_in.at[place], zsend.at[place], zrecv.at[place], (sp, place * 2 + core)
        ).wait_recv()
        out_ref[...] += z_in[place].astype(jnp.float32)
    for copy in swaps + sends:
        copy.wait_send()


def reduce_tp(x, tp_count, identity):
    block = x.shape[1:]
    depth = tp_count // 2
    buffer = pltpu.VMEM((depth,) + block, x.dtype)
    return comm_call(
        functools.partial(reduce_tp_kernel, tp_count),
        jax.ShapeDtypeStruct(block, jnp.float32),
        [buffer, buffer, buffer] + [pltpu.SemaphoreType.DMA((depth,))] * 4,
        identity,
        (x,),
    )


def swap_sp_kernel(sp_count, x_ref, out_ref, send, recv, local_sem):
    me = lax.axis_index("sp")
    tp = lax.axis_index("tp")
    others = [lax.rem(me + k, sp_count) for k in range(1, sp_count)]
    greet([(other, tp) for other in others])
    copies = []
    for other in others:
        copy = remote(x_ref.at[other], out_ref.at[me], send.at[other], recv.at[me], (other, tp))
        copy.start()
        copies.append(copy)
    own = pltpu.make_async_copy(x_ref.at[me], out_ref.at[me], local_sem)
    own.start()
    own.wait()
    for other in others:
        remote(
            x_ref.at[other], out_ref.at[other], send.at[other], recv.at[other], (other, tp)
        ).wait_recv()
    for copy in copies:
        copy.wait_send()


def swap_sp(x, sp_count, identity):
    return comm_call(
        functools.partial(swap_sp_kernel, sp_count),
        jax.ShapeDtypeStruct(x.shape, x.dtype),
        [
            pltpu.SemaphoreType.DMA((sp_count,)),
            pltpu.SemaphoreType.DMA((sp_count,)),
            pltpu.SemaphoreType.DMA,
        ],
        identity,
        (x,),
    )


NT = (((1,), (1,)), ((), ()))


def attend_kernel(
    rope_width,
    x_ref,
    q_ref,
    qr_ref,
    cos_ref,
    sin_ref,
    turn_ref,
    wk_ref,
    wv_ref,
    wo_ref,
    out_ref,
    turned,
    keys,
    values,
    tops,
    sums,
    acc,
):
    me = lax.axis_index("sp")
    tokens, width = q_ref.shape
    latent = wk_ref.shape[0]
    pair_width = width // (qr_ref.shape[1] // (2 * rope_width))
    pairs = width // pair_width
    raw = qr_ref[...]
    swapped = jnp.dot(raw, turn_ref[...], preferred_element_type=jnp.float32)
    turned[...] = (raw.astype(jnp.float32) * cos_ref[...] + swapped * sin_ref[...]).astype(
        turned.dtype
    )
    scales = ((DK_A + rope_width) ** (-0.5), (pair_width - DK_A + rope_width) ** (-0.5))

    def block(index, first):
        compressed = x_ref[index, :, :latent]
        rope = x_ref[index, :, latent:]
        keys[...] = jnp.dot(compressed, wk_ref[...], preferred_element_type=jnp.float32).astype(
            keys.dtype
        )
        values[...] = jnp.dot(compressed, wv_ref[...], preferred_element_type=jnp.float32).astype(
            values.dtype
        )
        for pair in range(pairs):
            span = slice(pair * pair_width, (pair + 1) * pair_width)
            lane = lax.broadcasted_iota(jnp.int32, (tokens, pair_width), 1)
            rope_lane = lax.broadcasted_iota(jnp.int32, turned.shape, 1)
            factors, updates = [], []
            for group in range(2):
                head = pair * 2 + group
                chosen = (lane < DK_A) if group == 0 else (lane >= DK_A)
                query = jnp.where(chosen, q_ref[:, span], jnp.zeros((), q_ref.dtype))
                low = head * rope_width
                query_rope = jnp.where(
                    (rope_lane >= low) & (rope_lane < low + rope_width),
                    turned[...],
                    jnp.zeros((), turned.dtype),
                )
                scores = lax.dot_general(
                    query, keys[:, span], NT, preferred_element_type=jnp.float32
                ) + lax.dot_general(query_rope, rope, NT, preferred_element_type=jnp.float32)
                scores = scores * scales[group]
                if first:
                    row = lax.broadcasted_iota(jnp.int32, (tokens, tokens), 0)
                    column = lax.broadcasted_iota(jnp.int32, (tokens, tokens), 1)
                    scores = jnp.where(row >= column, scores, floor_score)
                    top = jnp.max(scores, axis=1, keepdims=True)
                else:
                    old = tops[head]
                    top = jnp.maximum(old, jnp.max(scores, axis=1, keepdims=True))
                    factors.append(jnp.exp(old - top))
                weights = jnp.exp(scores - top)
                total = jnp.sum(weights, axis=1, keepdims=True)
                tops[head] = top
                sums[head] = total if first else sums[head] * factors[-1] + total
                updates.append(
                    jnp.dot(
                        weights.astype(values.dtype),
                        values[:, span],
                        preferred_element_type=jnp.float32,
                    )
                )
            value_lane = lane < DV_A
            update = jnp.where(value_lane, updates[0], updates[1])
            if first:
                acc[:, span] = update
            else:
                acc[:, span] = (
                    acc[:, span] * jnp.where(value_lane, factors[0], factors[1]) + update
                )

    block(me, True)

    def step(index, unused):
        block(index, False)
        return unused

    lax.fori_loop(0, me, step, 0)
    for pair in range(pairs):
        span = slice(pair * pair_width, (pair + 1) * pair_width)
        lane = lax.broadcasted_iota(jnp.int32, (tokens, pair_width), 1)
        bottom = jnp.where(lane < DV_A, sums[pair * 2], sums[pair * 2 + 1])
        keys[:, span] = (acc[:, span] / bottom).astype(keys.dtype)
    piece = 512
    for start in range(0, wo_ref.shape[1], piece):
        out_ref[:, start : start + piece] = jnp.dot(
            keys[...], wo_ref[:, start : start + piece], preferred_element_type=jnp.float32
        ).astype(out_ref.dtype)


def local(
    residual,
    queries,
    query_rope,
    latent,
    key_rope,
    latent_gain,
    key_weight,
    value_weight,
    out_weight,
    norm_gain,
    routes,
    group_gate,
    expert_share,
    gate_weight,
    up_weight,
    down_weight,
):
    tokens = queries.shape[0]
    pair_dev = queries.shape[1]
    sp_count = lax.axis_size("sp")
    tp_count = lax.axis_size("tp")
    row_count = tokens // tp_count
    rope_width = key_rope.shape[1]
    half = rope_width // 2
    copies = pair_dev * 2
    latent_width = latent.shape[1]
    model = residual.shape[1]
    low = jnp.bfloat16

    first_place = lax.axis_index("sp") * tokens
    places = (first_place + jnp.arange(tokens, dtype=jnp.int32)).astype(jnp.float32)
    cosine, sine = angle_tables(places, rope_width)
    cosine = jnp.tile(cosine, (1, 2 * copies))
    sine = jnp.tile(sine, (1, 2 * copies))
    index = jnp.arange(copies * rope_width, dtype=jnp.int32)
    source = jnp.where(index % rope_width < half, index + half, index - half)
    sign = jnp.where(index % rope_width < half, -1.0, 1.0)
    turn = jnp.where(index[:, None] == source[None, :], sign[None, :], 0.0).astype(low)
    key_raw = jnp.tile(key_rope, (1, copies))
    rotated = (
        key_raw.astype(jnp.float32) * cosine
        + jnp.dot(key_raw, turn, preferred_element_type=jnp.float32) * sine
    ).astype(low)
    compressed = rms_scale(latent, latent_gain).astype(low)
    gathered = gather_sp(jnp.concatenate([compressed, rotated], axis=1), sp_count, 0)

    width = pair_dev * queries.shape[2]
    scratch = [
        pltpu.VMEM((tokens, copies * rope_width), low),
        pltpu.VMEM((tokens, width), low),
        pltpu.VMEM((tokens, width), low),
        pltpu.VMEM((copies, tokens, 1), jnp.float32),
        pltpu.VMEM((copies, tokens, 1), jnp.float32),
        pltpu.VMEM((tokens, width), jnp.float32),
    ]
    partial = pl.pallas_call(
        functools.partial(attend_kernel, rope_width),
        out_shape=jax.ShapeDtypeStruct((tokens, model), low),
        in_specs=[VM] * 9,
        out_specs=VM,
        scratch_shapes=scratch,
        compiler_params=pltpu.CompilerParams(vmem_limit_bytes=56 * 1024 * 1024),
    )(
        gathered,
        queries.reshape(tokens, width),
        query_rope.reshape(tokens, copies * rope_width),
        cosine,
        sine,
        turn,
        key_weight.reshape(latent_width, -1),
        value_weight.reshape(latent_width, -1),
        out_weight.reshape(width, model),
    )
    head_total = reduce_tp(partial.reshape(tp_count, row_count, model), tp_count, 1)
    mixed_rows = residual.astype(jnp.float32) + head_total
    normed = rms_scale(mixed_rows, norm_gain).astype(low)

    experts_dev = gate_weight.shape[0]
    experts_all = experts_dev * sp_count
    top_count = routes.shape[1]
    capacity = max(2, 3 * row_count * top_count // (2 * experts_all))
    slots = experts_dev * capacity
    if experts_all // GROUPS == experts_dev == top_count:
        slots = capacity
    own = lax.dynamic_slice_in_dim(routes, lax.axis_index("tp") * row_count, row_count, 0)
    route_weight = group_gate[:, None] * expert_share / jnp.sum(expert_share, axis=1, keepdims=True)
    expert_ids = jnp.arange(experts_all, dtype=jnp.int32)
    named = own[:, :, None] == expert_ids[None, None, :]
    table = jnp.sum(jnp.where(named, route_weight[:, :, None], 0.0), axis=1)
    member = jnp.any(named, axis=1).reshape(row_count, sp_count, experts_dev).any(axis=2)
    counted = member.astype(jnp.int32)
    rank = jnp.cumsum(counted, axis=0) - counted
    slot_ids = jnp.arange(slots, dtype=jnp.int32)
    pick = (rank.T[:, None, :] == slot_ids[None, :, None]) & member.T[:, None, :]
    slot_weight = jnp.sum(
        jnp.where(
            pick[:, :, None, :],
            table.reshape(row_count, sp_count, experts_dev).transpose(1, 2, 0)[:, None],
            0.0,
        ),
        axis=3,
    )
    weight_high = slot_weight.astype(low)
    weight_low = (slot_weight - weight_high.astype(jnp.float32)).astype(low)
    pick_matrix = pick.astype(low).reshape(sp_count * slots, row_count)
    outgoing = jnp.dot(pick_matrix, normed, preferred_element_type=jnp.float32).astype(low)
    extra = jnp.concatenate([weight_high, weight_low], axis=2)
    extra = jnp.pad(extra, ((0, 0), (0, 0), (0, 128 - extra.shape[2])))
    outgoing = jnp.concatenate([outgoing.reshape(sp_count, slots, model), extra], axis=2)
    arrived = swap_sp(outgoing, sp_count, 2)
    rows = sp_count * slots
    everyone = gather_tp(arrived.reshape(rows, model + 128), tp_count, 3)
    everyone = everyone.reshape(tp_count * rows, model + 128)
    inputs = everyone[:, :model]
    tail = everyone[:, model : model + 2 * experts_dev].astype(jnp.float32)
    scale = tail[:, :experts_dev] + tail[:, experts_dev:]
    gate_out = jnp.einsum("rd,edf->erf", inputs, gate_weight, preferred_element_type=jnp.float32)
    up_out = jnp.einsum("rd,edf->erf", inputs, up_weight, preferred_element_type=jnp.float32)
    hidden = (jax.nn.silu(gate_out) * up_out * scale.T[:, :, None]).astype(low)
    expert_part = jnp.einsum(
        "erf,efd->rd", hidden, down_weight, preferred_element_type=jnp.float32
    ).astype(low)
    expert_out = reduce_tp(expert_part.reshape(tp_count, rows, model), tp_count, 4).astype(low)
    returned = swap_sp(expert_out.reshape(sp_count, slots, model), sp_count, 5)
    expert_mix = jnp.dot(
        pick_matrix.T, returned.reshape(rows, model), preferred_element_type=jnp.float32
    )
    return (mixed_rows + expert_mix).astype(low)


def solution(mesh):
    return jax.shard_map(
        local,
        mesh=mesh,
        in_specs=(
            P(("sp", "tp"), None),
            P("sp", "tp", None),
            P("sp", "tp", None),
            P("sp", None),
            P("sp", None),
            P(),
            P(None, "tp", None),
            P(None, "tp", None),
            P("tp", None, None),
            P(),
            P("sp", None),
            P(("sp", "tp")),
            P(("sp", "tp"), None),
            P("sp", None, "tp"),
            P("sp", None, "tp"),
            P("sp", "tp", None),
        ),
        out_specs=P(("sp", "tp"), None),
        check_vma=False,
    )
```

```python
import functools

import jax
import jax.numpy as jnp
from jax import lax
from jax.experimental import pallas as pl
from jax.experimental.pallas import tpu as pltpu
from jax.sharding import PartitionSpec as P

DK_A = 64
DV_A = 64
GROUPS = 4

rope_base = 10000.0
epsilon = 1e-06
floor_score = -1e30
MESH = pl.DeviceIdType.MESH
VM = pl.BlockSpec(memory_space=pltpu.VMEM)


def angle_tables(places, rope_width):
    frequencies = rope_base ** (-jnp.arange(0, rope_width, 2, dtype=jnp.float32) / rope_width)
    angles = places[:, None] * frequencies[None, :]
    return (jnp.cos(angles), jnp.sin(angles))


def rms_scale(values, gain_vector):
    values = values.astype(jnp.float32)
    inverse = lax.rsqrt(jnp.mean(values * values, axis=-1, keepdims=True) + epsilon)
    return values * inverse * gain_vector


def greet(targets):
    barrier = pltpu.get_barrier_semaphore()
    for target in targets:
        pl.semaphore_signal(barrier, inc=1, device_id=target, device_id_type=MESH)
    pl.semaphore_wait(barrier, len(targets))


def remote(src, dst, send, recv, target):
    return pltpu.make_async_remote_copy(
        src_ref=src,
        dst_ref=dst,
        send_sem=send,
        recv_sem=recv,
        device_id=target,
        device_id_type=MESH,
    )


def comm_call(kernel, out_shape, scratch, identity, args):
    return pl.pallas_call(
        kernel,
        out_shape=out_shape,
        in_specs=[VM] * len(args),
        out_specs=VM,
        scratch_shapes=scratch,
        compiler_params=pltpu.CompilerParams(
            collective_id=identity, has_side_effects=True, vmem_limit_bytes=48 * 1024 * 1024
        ),
    )(*args)


def greet_some(targets):
    barrier = pltpu.get_barrier_semaphore()
    count = 0
    for here, target in targets:

        @pl.when(here)
        def _():
            pl.semaphore_signal(barrier, inc=1, device_id=target, device_id_type=MESH)

        count = count + jnp.where(here, 1, 0)
    pl.semaphore_wait(barrier, count)


def line(tp_count):
    sp = lax.axis_index("sp")
    tp = lax.axis_index("tp")
    core = lax.rem(tp, 2)
    z = lax.div(tp, 2)
    depth = tp_count // 2
    partner = (sp, tp + 1 - 2 * core)
    return sp, core, z, depth, partner, (sp, tp + 2), (sp, tp - 2), z < depth - 1, z > 0


def expert_kernel(
    tp_count,
    x_ref,
    gate_ref,
    up_ref,
    down_ref,
    out_ref,
    held,
    gate,
    up,
    down,
    usend,
    dsend,
    psend,
    recv,
    wsem,
):
    sp, core, z, depth, partner, above, below, has_above, has_below = line(tp_count)
    tp = lax.axis_index("tp")
    experts = gate_ref.shape[0]
    model = gate_ref.shape[1]
    rows = x_ref.shape[0]
    loads = [
        pltpu.make_async_copy(source, target, wsem.at[i])
        for i, (source, target) in enumerate(((gate_ref, gate), (up_ref, up), (down_ref, down)))
    ]
    for load in loads:
        load.start()
    greet_some([(True, partner), (has_above, above), (has_below, below)])

    def move(block, sem, target, source=None):
        source = held.at[block] if source is None else source
        return remote(source, held.at[block], sem, recv.at[block], target)

    @pl.when(has_above)
    def _():
        move(tp, usend.at[z], above, x_ref).start()

    @pl.when(has_below)
    def _():
        move(tp, dsend.at[z], below, x_ref).start()

    move(tp, psend.at[z], partner, x_ref).start()
    held[tp] = x_ref[...]

    def take(k):
        low, high = z - k, z + k

        @pl.when(low >= 0)
        def _():
            block = low * 2 + core
            move(block, usend.at[low], partner).wait_recv()

            @pl.when(has_above)
            def _():
                move(block, usend.at[low], above).start()

            move(block, psend.at[low], partner).start()

        @pl.when(high < depth)
        def _():
            block = high * 2 + core
            move(block, dsend.at[high], partner).wait_recv()

            @pl.when(has_below)
            def _():
                move(block, dsend.at[high], below).start()

            move(block, psend.at[high], partner).start()

    def compute(place):
        move(place * 2 + 1 - core, psend.at[place], partner).wait_recv()
        blocks = pl.ds(place * 2, 2)
        x = held[blocks].reshape(2 * rows, held.shape[2])
        inputs = x[:, :model]
        tail = x[:, model:].astype(jnp.float32)
        total = None
        for e in range(experts):
            scale = tail[:, e : e + 1] + tail[:, experts + e : experts + e + 1]
            gate_out = jnp.dot(inputs, gate[e], preferred_element_type=jnp.float32)
            up_out = jnp.dot(inputs, up[e], preferred_element_type=jnp.float32)
            hidden = (jax.nn.silu(gate_out) * up_out * scale).astype(inputs.dtype)
            part = jnp.dot(hidden, down[e], preferred_element_type=jnp.float32)
            total = part if e == 0 else total + part
        out_ref[blocks] = total.astype(out_ref.dtype).reshape(2, rows, model)

    if depth > 1:
        take(1)
    for load in loads:
        load.wait()

    side = jnp.where(z * 2 >= depth, -1, 1)

    def step(k, unused):
        one, two = z + side * k, z - side * k

        @pl.when((one >= 0) & (one < depth))
        def _():
            compute(one)

        @pl.when((k > 0) & (k + 1 < depth))
        def _():
            take(k + 1)

        @pl.when((k > 0) & (two >= 0) & (two < depth))
        def _():
            compute(two)

        return unused

    lax.fori_loop(0, depth, step, 0)
    for place in range(depth):

        @pl.when(has_above & (place <= z))
        def _():
            move(place * 2 + core, usend.at[place], above).wait_send()

        @pl.when(has_below & (place >= z))
        def _():
            move(place * 2 + core, dsend.at[place], below).wait_send()

        move(place * 2 + core, psend.at[place], partner).wait_send()


def experts_over_tp(x, gate_weight, up_weight, down_weight, tp_count, identity):
    dma = pltpu.SemaphoreType.DMA
    depth = tp_count // 2
    model = gate_weight.shape[1]
    anywhere = pl.BlockSpec(memory_space=pl.ANY)
    return pl.pallas_call(
        functools.partial(expert_kernel, tp_count),
        out_shape=jax.ShapeDtypeStruct((tp_count, x.shape[0], model), x.dtype),
        in_specs=[VM, anywhere, anywhere, anywhere],
        out_specs=VM,
        scratch_shapes=[
            pltpu.VMEM((tp_count,) + x.shape, x.dtype),
            pltpu.VMEM(gate_weight.shape, gate_weight.dtype),
            pltpu.VMEM(up_weight.shape, up_weight.dtype),
            pltpu.VMEM(down_weight.shape, down_weight.dtype),
            dma((depth,)),
            dma((depth,)),
            dma((depth,)),
            dma((tp_count,)),
            dma((3,)),
        ],
        compiler_params=pltpu.CompilerParams(
            collective_id=identity, has_side_effects=True, vmem_limit_bytes=48 * 1024 * 1024
        ),
    )(x, gate_weight, up_weight, down_weight)


def reduce_tp_kernel(
    tp_count, x_ref, out_ref, partner_in, stage, up_in, down_in, send, recv, zsend, urecv, drecv
):
    sp, core, z, depth, partner, above, below, has_above, has_below = line(tp_count)
    greet_some([(True, partner), (has_above, above), (has_below, below)])

    def swap(place):
        return remote(
            x_ref.at[place * 2 + 1 - core],
            partner_in.at[place],
            send.at[place],
            recv.at[place],
            partner,
        )

    def up(place):
        return remote(
            stage.at[place], up_in.at[place], zsend.at[place], urecv.at[place], above
        )

    def down(place):
        return remote(
            stage.at[place], down_in.at[place], zsend.at[place], drecv.at[place], below
        )

    def pair_sum(place):
        swap(place).wait_recv()
        return x_ref[place * 2 + core].astype(jnp.float32) + partner_in[place].astype(jnp.float32)

    for j in range(depth):
        swap(depth - 1 - j).start()
        if depth - 1 - j > j:
            swap(j).start()
        if depth - 1 - j <= j + 1:
            break

    for j in range(depth - 1):
        high, low = depth - 1 + z - j, j + z + 1 - depth

        @pl.when(z <= j)
        def _():
            stage[high] = pair_sum(high).astype(stage.dtype)

            @pl.when(has_below)
            def _():
                up(high).wait_recv()
                stage[high] = (
                    stage[high].astype(jnp.float32) + up_in[high].astype(jnp.float32)
                ).astype(stage.dtype)

            up(high).start()

        @pl.when(low >= 0)
        def _():
            stage[low] = pair_sum(low).astype(stage.dtype)

            @pl.when(has_above)
            def _():
                down(low).wait_recv()
                stage[low] = (
                    stage[low].astype(jnp.float32) + down_in[low].astype(jnp.float32)
                ).astype(stage.dtype)

            down(low).start()

    out_ref[...] = pair_sum(z)

    @pl.when(has_below)
    def _():
        up(z).wait_recv()
        out_ref[...] += up_in[z].astype(jnp.float32)

    @pl.when(has_above)
    def _():
        down(z).wait_recv()
        out_ref[...] += down_in[z].astype(jnp.float32)

    for place in range(depth):
        swap(place).wait_send()

        @pl.when(place > z)
        def _():
            up(place).wait_send()

        @pl.when(place < z)
        def _():
            down(place).wait_send()


def reduce_tp(x, tp_count, identity):
    block = x.shape[1:]
    depth = tp_count // 2
    buffer = pltpu.VMEM((depth,) + block, x.dtype)
    return comm_call(
        functools.partial(reduce_tp_kernel, tp_count),
        jax.ShapeDtypeStruct(block, jnp.float32),
        [buffer] * 4 + [pltpu.SemaphoreType.DMA((depth,))] * 5,
        identity,
        (x,),
    )


def swap_sp_kernel(sp_count, x_ref, out_ref, send, recv, local_sem):
    me = lax.axis_index("sp")
    tp = lax.axis_index("tp")
    others = [lax.rem(me + k, sp_count) for k in range(1, sp_count)]
    greet([(other, tp) for other in others])
    copies = []
    for other in others:
        copy = remote(x_ref.at[other], out_ref.at[me], send.at[other], recv.at[me], (other, tp))
        copy.start()
        copies.append(copy)
    own = pltpu.make_async_copy(x_ref.at[me], out_ref.at[me], local_sem)
    own.start()
    own.wait()
    for other in others:
        remote(
            x_ref.at[other], out_ref.at[other], send.at[other], recv.at[other], (other, tp)
        ).wait_recv()
    for copy in copies:
        copy.wait_send()


def swap_sp(x, sp_count, identity):
    return comm_call(
        functools.partial(swap_sp_kernel, sp_count),
        jax.ShapeDtypeStruct(x.shape, x.dtype),
        [
            pltpu.SemaphoreType.DMA((sp_count,)),
            pltpu.SemaphoreType.DMA((sp_count,)),
            pltpu.SemaphoreType.DMA,
        ],
        identity,
        (x,),
    )


NT = (((1,), (1,)), ((), ()))


def attend_kernel(
    rope_width,
    sp_count,
    x_ref,
    q_ref,
    qr_ref,
    cos_ref,
    sin_ref,
    turn_ref,
    wk_ref,
    wv_ref,
    wo_ref,
    out_ref,
    turned,
    keys,
    values,
    tops,
    sums,
    acc,
    held,
    send,
    recv,
    fsend,
):
    me = lax.axis_index("sp")
    tp = lax.axis_index("tp")
    core = lax.rem(tp, 2)
    partner = (me, tp + 1 - 2 * core)
    tokens, width = q_ref.shape
    half = tokens // 2
    greet([(lax.rem(me + k, sp_count), tp) for k in range(1, sp_count)] + [partner])
    mine = pl.ds(pl.multiple_of(core * half, half), half)
    other = pl.ds(pl.multiple_of((1 - core) * half, half), half)

    def outgoing(to):
        return remote(
            x_ref.at[mine], held.at[me, mine], send.at[to], recv.at[me, core], (to, tp)
        )

    def incoming(source):
        return remote(
            x_ref.at[mine], held.at[source, mine], send.at[source], recv.at[source, core], partner
        )

    def forward(source):
        return remote(
            held.at[source, mine],
            held.at[source, mine],
            fsend.at[source],
            recv.at[source, core],
            partner,
        )

    def forwarded(source):
        return remote(
            held.at[source, other],
            held.at[source, other],
            fsend.at[source],
            recv.at[source, 1 - core],
            partner,
        )

    for to in reversed(range(sp_count)):

        @pl.when(to > me)
        def _():
            outgoing(to).start()

    latent = wk_ref.shape[0]
    pair_width = width // (qr_ref.shape[1] // (2 * rope_width))
    pairs = width // pair_width
    raw = qr_ref[...]
    swapped = jnp.dot(raw, turn_ref[...], preferred_element_type=jnp.float32)
    turned[...] = (raw.astype(jnp.float32) * cos_ref[...] + swapped * sin_ref[...]).astype(
        turned.dtype
    )
    scales = ((DK_A + rope_width) ** (-0.5), (pair_width - DK_A + rope_width) ** (-0.5))

    def block(index, first):
        compressed = x_ref[:, :latent] if first else held[index, :, :latent]
        rope = x_ref[:, latent:] if first else held[index, :, latent:]
        keys[...] = jnp.dot(compressed, wk_ref[...], preferred_element_type=jnp.float32).astype(
            keys.dtype
        )
        values[...] = jnp.dot(compressed, wv_ref[...], preferred_element_type=jnp.float32).astype(
            values.dtype
        )
        for pair in range(pairs):
            span = slice(pair * pair_width, (pair + 1) * pair_width)
            lane = lax.broadcasted_iota(jnp.int32, (tokens, pair_width), 1)
            rope_lane = lax.broadcasted_iota(jnp.int32, turned.shape, 1)
            factors, updates = [], []
            for group in range(2):
                head = pair * 2 + group
                chosen = (lane < DK_A) if group == 0 else (lane >= DK_A)
                query = jnp.where(chosen, q_ref[:, span], jnp.zeros((), q_ref.dtype))
                low = head * rope_width
                query_rope = jnp.where(
                    (rope_lane >= low) & (rope_lane < low + rope_width),
                    turned[...],
                    jnp.zeros((), turned.dtype),
                )
                scores = lax.dot_general(
                    query, keys[:, span], NT, preferred_element_type=jnp.float32
                ) + lax.dot_general(query_rope, rope, NT, preferred_element_type=jnp.float32)
                scores = scores * scales[group]
                if first:
                    row = lax.broadcasted_iota(jnp.int32, (tokens, tokens), 0)
                    column = lax.broadcasted_iota(jnp.int32, (tokens, tokens), 1)
                    scores = jnp.where(row >= column, scores, floor_score)
                    top = jnp.max(scores, axis=1, keepdims=True)
                else:
                    old = tops[head]
                    top = jnp.maximum(old, jnp.max(scores, axis=1, keepdims=True))
                    factors.append(jnp.exp(old - top))
                weights = jnp.exp(scores - top)
                total = jnp.sum(weights, axis=1, keepdims=True)
                tops[head] = top
                sums[head] = total if first else sums[head] * factors[-1] + total
                updates.append(
                    jnp.dot(
                        weights.astype(values.dtype),
                        values[:, span],
                        preferred_element_type=jnp.float32,
                    )
                )
            value_lane = lane < DV_A
            update = jnp.where(value_lane, updates[0], updates[1])
            if first:
                acc[:, span] = update
            else:
                acc[:, span] = (
                    acc[:, span] * jnp.where(value_lane, factors[0], factors[1]) + update
                )

    block(me, True)

    def step(i, unused):
        index = me - 1 - i
        incoming(index).wait_recv()
        forward(index).start()
        forwarded(index).wait_recv()
        block(index, False)
        return unused

    lax.fori_loop(0, me, step, 0)
    for pair in range(pairs):
        span = slice(pair * pair_width, (pair + 1) * pair_width)
        lane = lax.broadcasted_iota(jnp.int32, (tokens, pair_width), 1)
        bottom = jnp.where(lane < DV_A, sums[pair * 2], sums[pair * 2 + 1])
        keys[:, span] = (acc[:, span] / bottom).astype(keys.dtype)
    piece = 512
    for start in range(0, wo_ref.shape[1], piece):
        out_ref[:, start : start + piece] = jnp.dot(
            keys[...], wo_ref[:, start : start + piece], preferred_element_type=jnp.float32
        ).astype(out_ref.dtype)
    for place in range(sp_count):

        @pl.when(place < me)
        def _():
            forward(place).wait_send()

        @pl.when(place > me)
        def _():
            outgoing(place).wait_send()


def local(
    residual,
    queries,
    query_rope,
    latent,
    key_rope,
    latent_gain,
    key_weight,
    value_weight,
    out_weight,
    norm_gain,
    routes,
    group_gate,
    expert_share,
    gate_weight,
    up_weight,
    down_weight,
):
    tokens = queries.shape[0]
    pair_dev = queries.shape[1]
    sp_count = lax.axis_size("sp")
    tp_count = lax.axis_size("tp")
    row_count = tokens // tp_count
    rope_width = key_rope.shape[1]
    half = rope_width // 2
    copies = pair_dev * 2
    latent_width = latent.shape[1]
    model = residual.shape[1]
    low = jnp.bfloat16

    first_place = lax.axis_index("sp") * tokens
    places = (first_place + jnp.arange(tokens, dtype=jnp.int32)).astype(jnp.float32)
    cosine, sine = angle_tables(places, rope_width)
    cosine = jnp.tile(cosine, (1, 2 * copies))
    sine = jnp.tile(sine, (1, 2 * copies))
    index = jnp.arange(copies * rope_width, dtype=jnp.int32)
    source = jnp.where(index % rope_width < half, index + half, index - half)
    sign = jnp.where(index % rope_width < half, -1.0, 1.0)
    turn = jnp.where(index[:, None] == source[None, :], sign[None, :], 0.0).astype(low)
    key_raw = jnp.tile(key_rope, (1, copies))
    rotated = (
        key_raw.astype(jnp.float32) * cosine
        + jnp.dot(key_raw, turn, preferred_element_type=jnp.float32) * sine
    ).astype(low)
    compressed = rms_scale(latent, latent_gain).astype(low)
    own_latent = jnp.concatenate([compressed, rotated], axis=1)

    width = pair_dev * queries.shape[2]
    scratch = [
        pltpu.VMEM((tokens, copies * rope_width), low),
        pltpu.VMEM((tokens, width), low),
        pltpu.VMEM((tokens, width), low),
        pltpu.VMEM((copies, tokens, 1), jnp.float32),
        pltpu.VMEM((copies, tokens, 1), jnp.float32),
        pltpu.VMEM((tokens, width), jnp.float32),
        pltpu.VMEM((sp_count,) + own_latent.shape, low),
        pltpu.SemaphoreType.DMA((sp_count,)),
        pltpu.SemaphoreType.DMA((sp_count, 2)),
        pltpu.SemaphoreType.DMA((sp_count,)),
    ]
    partial = pl.pallas_call(
        functools.partial(attend_kernel, rope_width, sp_count),
        out_shape=jax.ShapeDtypeStruct((tokens, model), low),
        in_specs=[VM] * 9,
        out_specs=VM,
        scratch_shapes=scratch,
        compiler_params=pltpu.CompilerParams(
            collective_id=0, has_side_effects=True, vmem_limit_bytes=48 * 1024 * 1024
        ),
    )(
        own_latent,
        queries.reshape(tokens, width),
        query_rope.reshape(tokens, copies * rope_width),
        cosine,
        sine,
        turn,
        key_weight.reshape(latent_width, -1),
        value_weight.reshape(latent_width, -1),
        out_weight.reshape(width, model),
    )
    head_total = reduce_tp(partial.reshape(tp_count, row_count, model), tp_count, 1)
    mixed_rows = residual.astype(jnp.float32) + head_total
    normed = rms_scale(mixed_rows, norm_gain).astype(low)

    experts_dev = gate_weight.shape[0]
    experts_all = experts_dev * sp_count
    top_count = routes.shape[1]
    capacity = max(2, 3 * row_count * top_count // (2 * experts_all))
    slots = experts_dev * capacity
    if experts_all // GROUPS == experts_dev == top_count:
        slots = capacity
    own = lax.dynamic_slice_in_dim(routes, lax.axis_index("tp") * row_count, row_count, 0)
    route_weight = group_gate[:, None] * expert_share / jnp.sum(expert_share, axis=1, keepdims=True)
    expert_ids = jnp.arange(experts_all, dtype=jnp.int32)
    named = own[:, :, None] == expert_ids[None, None, :]
    table = jnp.sum(jnp.where(named, route_weight[:, :, None], 0.0), axis=1)
    member = jnp.any(named, axis=1).reshape(row_count, sp_count, experts_dev).any(axis=2)
    counted = member.astype(jnp.int32)
    rank = jnp.cumsum(counted, axis=0) - counted
    slot_ids = jnp.arange(slots, dtype=jnp.int32)
    pick = (rank.T[:, None, :] == slot_ids[None, :, None]) & member.T[:, None, :]
    slot_weight = jnp.sum(
        jnp.where(
            pick[:, :, None, :],
            table.reshape(row_count, sp_count, experts_dev).transpose(1, 2, 0)[:, None],
            0.0,
        ),
        axis=3,
    )
    weight_high = slot_weight.astype(low)
    weight_low = (slot_weight - weight_high.astype(jnp.float32)).astype(low)
    pick_matrix = pick.astype(low).reshape(sp_count * slots, row_count)
    outgoing = jnp.dot(pick_matrix, normed, preferred_element_type=jnp.float32).astype(low)
    extra = jnp.concatenate([weight_high, weight_low], axis=2)
    extra = jnp.pad(extra, ((0, 0), (0, 0), (0, 128 - extra.shape[2])))
    outgoing = jnp.concatenate([outgoing.reshape(sp_count, slots, model), extra], axis=2)
    arrived = swap_sp(outgoing, sp_count, 2)
    rows = sp_count * slots
    expert_part = experts_over_tp(
        arrived.reshape(rows, model + 128), gate_weight, up_weight, down_weight, tp_count, 3
    )
    expert_out = reduce_tp(expert_part, tp_count, 4).astype(low)
    returned = swap_sp(expert_out.reshape(sp_count, slots, model), sp_count, 5)
    expert_mix = jnp.dot(
        pick_matrix.T, returned.reshape(rows, model), preferred_element_type=jnp.float32
    )
    return (mixed_rows + expert_mix).astype(low)


def solution(mesh):
    return jax.shard_map(
        local,
        mesh=mesh,
        in_specs=(
            P(("sp", "tp"), None),
            P("sp", "tp", None),
            P("sp", "tp", None),
            P("sp", None),
            P("sp", None),
            P(),
            P(None, "tp", None),
            P(None, "tp", None),
            P("tp", None, None),
            P(),
            P("sp", None),
            P(("sp", "tp")),
            P(("sp", "tp"), None),
            P("sp", None, "tp"),
            P("sp", None, "tp"),
            P("sp", "tp", None),
        ),
        out_specs=P(("sp", "tp"), None),
        check_vma=False,
    )
```

```python
import functools

import jax
import jax.numpy as jnp
from jax import lax
from jax.experimental import pallas as pl
from jax.experimental.pallas import tpu as pltpu
from jax.sharding import PartitionSpec as P

DK_A = 64
DV_A = 64
GROUPS = 4

rope_base = 10000.0
epsilon = 1e-06
floor_score = -1e30
MESH = pl.DeviceIdType.MESH
VM = pl.BlockSpec(memory_space=pltpu.VMEM)


def angle_tables(places, rope_width, repeats):
    steps = jnp.arange(repeats * rope_width // 2, dtype=jnp.int32) % (rope_width // 2)
    frequencies = rope_base ** (-(2 * steps).astype(jnp.float32) / rope_width)
    angles = places[:, None] * frequencies[None, :]
    return (jnp.cos(angles), jnp.sin(angles))


def rms_scale(values, gain_vector):
    values = values.astype(jnp.float32)
    inverse = lax.rsqrt(jnp.mean(values * values, axis=-1, keepdims=True) + epsilon)
    return values * inverse * gain_vector


def greet(targets):
    barrier = pltpu.get_barrier_semaphore()
    for target in targets:
        pl.semaphore_signal(barrier, inc=1, device_id=target, device_id_type=MESH)
    pl.semaphore_wait(barrier, len(targets))


def remote(src, dst, send, recv, target):
    return pltpu.make_async_remote_copy(
        src_ref=src,
        dst_ref=dst,
        send_sem=send,
        recv_sem=recv,
        device_id=target,
        device_id_type=MESH,
    )


def comm_call(kernel, out_shape, scratch, identity, args):
    return pl.pallas_call(
        kernel,
        out_shape=out_shape,
        in_specs=[VM] * len(args),
        out_specs=VM,
        scratch_shapes=scratch,
        compiler_params=pltpu.CompilerParams(
            collective_id=identity, has_side_effects=True, vmem_limit_bytes=48 * 1024 * 1024
        ),
    )(*args)


def greet_some(targets):
    barrier = pltpu.get_barrier_semaphore()
    count = 0
    for here, target in targets:

        @pl.when(here)
        def _():
            pl.semaphore_signal(barrier, inc=1, device_id=target, device_id_type=MESH)

        count = count + jnp.where(here, 1, 0)
    pl.semaphore_wait(barrier, count)


def line(tp_count):
    sp = lax.axis_index("sp")
    tp = lax.axis_index("tp")
    core = lax.rem(tp, 2)
    z = lax.div(tp, 2)
    depth = tp_count // 2
    partner = (sp, tp + 1 - 2 * core)
    return sp, core, z, depth, partner, (sp, tp + 2), (sp, tp - 2), z < depth - 1, z > 0


def expert_kernel(
    tp_count,
    x_ref,
    gate_ref,
    up_ref,
    down_ref,
    out_ref,
    held,
    gate,
    up,
    down,
    usend,
    dsend,
    psend,
    recv,
    wsem,
):
    sp, core, z, depth, partner, above, below, has_above, has_below = line(tp_count)
    tp = lax.axis_index("tp")
    experts = gate_ref.shape[0]
    model = gate_ref.shape[1]
    rows = x_ref.shape[0]
    middle = x_ref.shape[1] // 256 * 128
    parts = (slice(0, middle), slice(middle, x_ref.shape[1]))
    loads = [
        pltpu.make_async_copy(source, target, wsem.at[i])
        for i, (source, target) in enumerate(((gate_ref, gate), (up_ref, up), (down_ref, down)))
    ]
    for load in loads:
        load.start()
    greet_some([(True, partner), (has_above, above), (has_below, below)])

    def move(block, sems, place, part, target, source=None):
        source = held.at[block] if source is None else source
        return remote(
            source.at[:, parts[part]],
            held.at[block, :, parts[part]],
            sems.at[place, part],
            recv.at[block, part],
            target,
        )

    for part in range(2):

        @pl.when(has_above)
        def _():
            move(tp, usend, z, part, above, x_ref).start()

        @pl.when(has_below)
        def _():
            move(tp, dsend, z, part, below, x_ref).start()

        move(tp, psend, z, part, partner, x_ref).start()
    held[tp] = x_ref[...]

    def take(k):
        low, high = z - k, z + k
        for part in range(2):

            @pl.when(low >= 0)
            def _():
                block = low * 2 + core
                move(block, usend, low, part, partner).wait_recv()

                @pl.when(has_above)
                def _():
                    move(block, usend, low, part, above).start()

                move(block, psend, low, part, partner).start()

            @pl.when(high < depth)
            def _():
                block = high * 2 + core
                move(block, dsend, high, part, partner).wait_recv()

                @pl.when(has_below)
                def _():
                    move(block, dsend, high, part, below).start()

                move(block, psend, high, part, partner).start()

    def compute(place):
        for part in range(2):
            move(place * 2 + 1 - core, psend, place, part, partner).wait_recv()
        blocks = pl.ds(place * 2, 2)
        x = held[blocks].reshape(2 * rows, held.shape[2])
        inputs = x[:, :model]
        tail = x[:, model:].astype(jnp.float32)
        total = None
        for e in range(experts):
            scale = tail[:, e : e + 1] + tail[:, experts + e : experts + e + 1]
            gate_out = jnp.dot(inputs, gate[e], preferred_element_type=jnp.float32)
            up_out = jnp.dot(inputs, up[e], preferred_element_type=jnp.float32)
            hidden = (jax.nn.silu(gate_out) * up_out * scale).astype(inputs.dtype)
            part = jnp.dot(hidden, down[e], preferred_element_type=jnp.float32)
            total = part if e == 0 else total + part
        out_ref[blocks] = total.astype(out_ref.dtype).reshape(2, rows, model)

    if depth > 1:
        take(1)
    for load in loads:
        load.wait()

    side = jnp.where(z * 2 >= depth, -1, 1)

    def step(k, unused):
        one, two = z + side * k, z - side * k

        @pl.when((one >= 0) & (one < depth))
        def _():
            compute(one)

        @pl.when((k > 0) & (k + 1 < depth))
        def _():
            take(k + 1)

        @pl.when((k > 0) & (two >= 0) & (two < depth))
        def _():
            compute(two)

        return unused

    lax.fori_loop(0, depth, step, 0)
    for place in range(depth):
        for part in range(2):

            @pl.when(has_above & (place <= z))
            def _():
                move(place * 2 + core, usend, place, part, above).wait_send()

            @pl.when(has_below & (place >= z))
            def _():
                move(place * 2 + core, dsend, place, part, below).wait_send()

            move(place * 2 + core, psend, place, part, partner).wait_send()


def experts_over_tp(x, gate_weight, up_weight, down_weight, tp_count, identity):
    dma = pltpu.SemaphoreType.DMA
    depth = tp_count // 2
    model = gate_weight.shape[1]
    anywhere = pl.BlockSpec(memory_space=pl.ANY)
    return pl.pallas_call(
        functools.partial(expert_kernel, tp_count),
        out_shape=jax.ShapeDtypeStruct((tp_count, x.shape[0], model), x.dtype),
        in_specs=[VM, anywhere, anywhere, anywhere],
        out_specs=VM,
        scratch_shapes=[
            pltpu.VMEM((tp_count,) + x.shape, x.dtype),
            pltpu.VMEM(gate_weight.shape, gate_weight.dtype),
            pltpu.VMEM(up_weight.shape, up_weight.dtype),
            pltpu.VMEM(down_weight.shape, down_weight.dtype),
            dma((depth, 2)),
            dma((depth, 2)),
            dma((depth, 2)),
            dma((tp_count, 2)),
            dma((3,)),
        ],
        compiler_params=pltpu.CompilerParams(
            collective_id=identity, has_side_effects=True, vmem_limit_bytes=48 * 1024 * 1024
        ),
    )(x, gate_weight, up_weight, down_weight)


def reduce_tp_kernel(
    tp_count, x_ref, out_ref, partner_in, stage, up_in, down_in, send, recv, zsend, urecv, drecv
):
    sp, core, z, depth, partner, above, below, has_above, has_below = line(tp_count)
    greet_some([(True, partner), (has_above, above), (has_below, below)])

    middle = x_ref.shape[2] // 256 * 128
    parts = (slice(0, middle), slice(middle, x_ref.shape[2]))

    def swap(place, part):
        return remote(
            x_ref.at[place * 2 + 1 - core, :, parts[part]],
            partner_in.at[place, :, parts[part]],
            send.at[place, part],
            recv.at[place, part],
            partner,
        )

    def pass_on(place, part, arrivals, sems, target):
        return remote(
            stage.at[place, :, parts[part]],
            arrivals.at[place, :, parts[part]],
            zsend.at[place, part],
            sems.at[place, part],
            target,
        )

    def up(place, part):
        return pass_on(place, part, up_in, urecv, above)

    def down(place, part):
        return pass_on(place, part, down_in, drecv, below)

    def pair_sum(place, part):
        swap(place, part).wait_recv()
        mine = x_ref[place * 2 + core, :, parts[part]].astype(jnp.float32)
        return mine + partner_in[place, :, parts[part]].astype(jnp.float32)

    for j in range(depth):
        for part in range(2):
            swap(depth - 1 - j, part).start()
            if depth - 1 - j > j:
                swap(j, part).start()
        if depth - 1 - j <= j + 1:
            break

    for j in range(depth - 1):
        high, low = depth - 1 + z - j, j + z + 1 - depth
        for part in range(2):
            span = parts[part]

            @pl.when(z <= j)
            def _():
                stage[high, :, span] = pair_sum(high, part).astype(stage.dtype)

                @pl.when(has_below)
                def _():
                    up(high, part).wait_recv()
                    stage[high, :, span] = (
                        stage[high, :, span].astype(jnp.float32)
                        + up_in[high, :, span].astype(jnp.float32)
                    ).astype(stage.dtype)

                up(high, part).start()

            @pl.when(low >= 0)
            def _():
                stage[low, :, span] = pair_sum(low, part).astype(stage.dtype)

                @pl.when(has_above)
                def _():
                    down(low, part).wait_recv()
                    stage[low, :, span] = (
                        stage[low, :, span].astype(jnp.float32)
                        + down_in[low, :, span].astype(jnp.float32)
                    ).astype(stage.dtype)

                down(low, part).start()

    for part in range(2):
        span = parts[part]
        out_ref[:, span] = pair_sum(z, part)

        @pl.when(has_below)
        def _():
            up(z, part).wait_recv()
            out_ref[:, span] += up_in[z, :, span].astype(jnp.float32)

        @pl.when(has_above)
        def _():
            down(z, part).wait_recv()
            out_ref[:, span] += down_in[z, :, span].astype(jnp.float32)

    for place in range(depth):
        for part in range(2):
            swap(place, part).wait_send()

            @pl.when(place > z)
            def _():
                up(place, part).wait_send()

            @pl.when(place < z)
            def _():
                down(place, part).wait_send()


def reduce_tp(x, tp_count, identity):
    block = x.shape[1:]
    depth = tp_count // 2
    buffer = pltpu.VMEM((depth,) + block, x.dtype)
    return comm_call(
        functools.partial(reduce_tp_kernel, tp_count),
        jax.ShapeDtypeStruct(block, jnp.float32),
        [buffer] * 4 + [pltpu.SemaphoreType.DMA((depth, 2))] * 5,
        identity,
        (x,),
    )


def swap_sp_kernel(sp_count, x_ref, out_ref, send, recv, local_sem):
    me = lax.axis_index("sp")
    tp = lax.axis_index("tp")
    others = [lax.rem(me + k, sp_count) for k in range(1, sp_count)]
    greet([(other, tp) for other in others])
    copies = []
    for other in others:
        copy = remote(x_ref.at[other], out_ref.at[me], send.at[other], recv.at[me], (other, tp))
        copy.start()
        copies.append(copy)
    own = pltpu.make_async_copy(x_ref.at[me], out_ref.at[me], local_sem)
    own.start()
    own.wait()
    for other in others:
        remote(
            x_ref.at[other], out_ref.at[other], send.at[other], recv.at[other], (other, tp)
        ).wait_recv()
    for copy in copies:
        copy.wait_send()


def swap_sp(x, sp_count, identity):
    return comm_call(
        functools.partial(swap_sp_kernel, sp_count),
        jax.ShapeDtypeStruct(x.shape, x.dtype),
        [
            pltpu.SemaphoreType.DMA((sp_count,)),
            pltpu.SemaphoreType.DMA((sp_count,)),
            pltpu.SemaphoreType.DMA,
        ],
        identity,
        (x,),
    )


NT = (((1,), (1,)), ((), ()))


def attend_kernel(
    rope_width,
    sp_count,
    x_ref,
    q_ref,
    qr_ref,
    cos_ref,
    sin_ref,
    turn_ref,
    wk_ref,
    wv_ref,
    wo_ref,
    out_ref,
    turned,
    keys,
    values,
    tops,
    sums,
    acc,
    held,
    send,
    recv,
    fsend,
):
    me = lax.axis_index("sp")
    tp = lax.axis_index("tp")
    core = lax.rem(tp, 2)
    partner = (me, tp + 1 - 2 * core)
    tokens, width = q_ref.shape
    half = tokens // 2
    greet([(lax.rem(me + k, sp_count), tp) for k in range(1, sp_count)] + [partner])
    mine = pl.ds(pl.multiple_of(core * half, half), half)
    other = pl.ds(pl.multiple_of((1 - core) * half, half), half)

    def outgoing(to):
        return remote(
            x_ref.at[mine], held.at[me, mine], send.at[to], recv.at[me, core], (to, tp)
        )

    def incoming(source):
        return remote(
            x_ref.at[mine], held.at[source, mine], send.at[source], recv.at[source, core], partner
        )

    def forward(source):
        return remote(
            held.at[source, mine],
            held.at[source, mine],
            fsend.at[source],
            recv.at[source, core],
            partner,
        )

    def forwarded(source):
        return remote(
            held.at[source, other],
            held.at[source, other],
            fsend.at[source],
            recv.at[source, 1 - core],
            partner,
        )

    for to in reversed(range(sp_count)):

        @pl.when(to > me)
        def _():
            outgoing(to).start()

    latent = wk_ref.shape[0]
    pair_width = width // (qr_ref.shape[1] // (2 * rope_width))
    pairs = width // pair_width
    raw = qr_ref[...]
    swapped = jnp.dot(raw, turn_ref[...], preferred_element_type=jnp.float32)
    turned[...] = (raw.astype(jnp.float32) * cos_ref[...] + swapped * sin_ref[...]).astype(
        turned.dtype
    )
    scales = ((DK_A + rope_width) ** (-0.5), (pair_width - DK_A + rope_width) ** (-0.5))

    def block(index, first):
        compressed = x_ref[:, :latent] if first else held[index, :, :latent]
        rope = x_ref[:, latent:] if first else held[index, :, latent:]
        keys[...] = jnp.dot(compressed, wk_ref[...], preferred_element_type=jnp.float32).astype(
            keys.dtype
        )
        values[...] = jnp.dot(compressed, wv_ref[...], preferred_element_type=jnp.float32).astype(
            values.dtype
        )
        for pair in range(pairs):
            span = slice(pair * pair_width, (pair + 1) * pair_width)
            lane = lax.broadcasted_iota(jnp.int32, (tokens, pair_width), 1)
            rope_lane = lax.broadcasted_iota(jnp.int32, turned.shape, 1)
            factors, updates = [], []
            for group in range(2):
                head = pair * 2 + group
                chosen = (lane < DK_A) if group == 0 else (lane >= DK_A)
                query = jnp.where(chosen, q_ref[:, span], jnp.zeros((), q_ref.dtype))
                low = head * rope_width
                query_rope = jnp.where(
                    (rope_lane >= low) & (rope_lane < low + rope_width),
                    turned[...],
                    jnp.zeros((), turned.dtype),
                )
                scores = lax.dot_general(
                    query, keys[:, span], NT, preferred_element_type=jnp.float32
                ) + lax.dot_general(query_rope, rope, NT, preferred_element_type=jnp.float32)
                scores = scores * scales[group]
                if first:
                    row = lax.broadcasted_iota(jnp.int32, (tokens, tokens), 0)
                    column = lax.broadcasted_iota(jnp.int32, (tokens, tokens), 1)
                    scores = jnp.where(row >= column, scores, floor_score)
                    top = jnp.max(scores, axis=1, keepdims=True)
                else:
                    old = tops[head]
                    top = jnp.maximum(old, jnp.max(scores, axis=1, keepdims=True))
                    factors.append(jnp.exp(old - top))
                weights = jnp.exp(scores - top)
                total = jnp.sum(weights, axis=1, keepdims=True)
                tops[head] = top
                sums[head] = total if first else sums[head] * factors[-1] + total
                updates.append(
                    jnp.dot(
                        weights.astype(values.dtype),
                        values[:, span],
                        preferred_element_type=jnp.float32,
                    )
                )
            value_lane = lane < DV_A
            update = jnp.where(value_lane, updates[0], updates[1])
            if first:
                acc[:, span] = update
            else:
                acc[:, span] = (
                    acc[:, span] * jnp.where(value_lane, factors[0], factors[1]) + update
                )

    block(me, True)

    def step(i, unused):
        index = me - 1 - i
        incoming(index).wait_recv()
        forward(index).start()
        forwarded(index).wait_recv()
        block(index, False)
        return unused

    lax.fori_loop(0, me, step, 0)
    for pair in range(pairs):
        span = slice(pair * pair_width, (pair + 1) * pair_width)
        lane = lax.broadcasted_iota(jnp.int32, (tokens, pair_width), 1)
        bottom = jnp.where(lane < DV_A, sums[pair * 2], sums[pair * 2 + 1])
        keys[:, span] = (acc[:, span] / bottom).astype(keys.dtype)
    piece = 512
    for start in range(0, wo_ref.shape[1], piece):
        out_ref[:, start : start + piece] = jnp.dot(
            keys[...], wo_ref[:, start : start + piece], preferred_element_type=jnp.float32
        ).astype(out_ref.dtype)
    for place in range(sp_count):

        @pl.when(place < me)
        def _():
            forward(place).wait_send()

        @pl.when(place > me)
        def _():
            outgoing(place).wait_send()


def local(
    residual,
    queries,
    query_rope,
    latent,
    key_rope,
    latent_gain,
    key_weight,
    value_weight,
    out_weight,
    norm_gain,
    routes,
    group_gate,
    expert_share,
    gate_weight,
    up_weight,
    down_weight,
):
    tokens = queries.shape[0]
    pair_dev = queries.shape[1]
    sp_count = lax.axis_size("sp")
    tp_count = lax.axis_size("tp")
    row_count = tokens // tp_count
    rope_width = key_rope.shape[1]
    half = rope_width // 2
    copies = pair_dev * 2
    latent_width = latent.shape[1]
    model = residual.shape[1]
    low = jnp.bfloat16

    first_place = lax.axis_index("sp") * tokens
    places = (first_place + jnp.arange(tokens, dtype=jnp.int32)).astype(jnp.float32)
    cosine, sine = angle_tables(places, rope_width, 2 * copies)
    index = jnp.arange(copies * rope_width, dtype=jnp.int32)
    source = jnp.where(index % rope_width < half, index + half, index - half)
    sign = jnp.where(index % rope_width < half, -1.0, 1.0)
    turn = jnp.where(index[:, None] == source[None, :], sign[None, :], 0.0).astype(low)
    key_raw = jnp.tile(key_rope, (1, copies))
    rotated = (
        key_raw.astype(jnp.float32) * cosine
        + jnp.dot(key_raw, turn, preferred_element_type=jnp.float32) * sine
    ).astype(low)
    compressed = rms_scale(latent, latent_gain).astype(low)
    own_latent = jnp.concatenate([compressed, rotated], axis=1)

    width = pair_dev * queries.shape[2]
    scratch = [
        pltpu.VMEM((tokens, copies * rope_width), low),
        pltpu.VMEM((tokens, width), low),
        pltpu.VMEM((tokens, width), low),
        pltpu.VMEM((copies, tokens, 1), jnp.float32),
        pltpu.VMEM((copies, tokens, 1), jnp.float32),
        pltpu.VMEM((tokens, width), jnp.float32),
        pltpu.VMEM((sp_count,) + own_latent.shape, low),
        pltpu.SemaphoreType.DMA((sp_count,)),
        pltpu.SemaphoreType.DMA((sp_count, 2)),
        pltpu.SemaphoreType.DMA((sp_count,)),
    ]
    partial = pl.pallas_call(
        functools.partial(attend_kernel, rope_width, sp_count),
        out_shape=jax.ShapeDtypeStruct((tokens, model), low),
        in_specs=[VM] * 9,
        out_specs=VM,
        scratch_shapes=scratch,
        compiler_params=pltpu.CompilerParams(
            collective_id=0, has_side_effects=True, vmem_limit_bytes=48 * 1024 * 1024
        ),
    )(
        own_latent,
        queries.reshape(tokens, width),
        query_rope.reshape(tokens, copies * rope_width),
        cosine,
        sine,
        turn,
        key_weight.reshape(latent_width, -1),
        value_weight.reshape(latent_width, -1),
        out_weight.reshape(width, model),
    )
    head_total = reduce_tp(partial.reshape(tp_count, row_count, model), tp_count, 1)
    mixed_rows = residual.astype(jnp.float32) + head_total
    normed = rms_scale(mixed_rows, norm_gain).astype(low)

    experts_dev = gate_weight.shape[0]
    experts_all = experts_dev * sp_count
    top_count = routes.shape[1]
    capacity = max(2, 3 * row_count * top_count // (2 * experts_all))
    slots = experts_dev * capacity
    if experts_all // GROUPS == experts_dev == top_count:
        slots = capacity
    own = lax.dynamic_slice_in_dim(routes, lax.axis_index("tp") * row_count, row_count, 0)
    route_weight = group_gate[:, None] * expert_share / jnp.sum(expert_share, axis=1, keepdims=True)
    expert_ids = jnp.arange(experts_all, dtype=jnp.int32)
    named = own[:, :, None] == expert_ids[None, None, :]
    table = jnp.sum(jnp.where(named, route_weight[:, :, None], 0.0), axis=1)
    member = jnp.any(named, axis=1).reshape(row_count, sp_count, experts_dev).any(axis=2)
    counted = member.astype(jnp.int32)
    rank = jnp.cumsum(counted, axis=0) - counted
    slot_ids = jnp.arange(slots, dtype=jnp.int32)
    pick = (rank.T[:, None, :] == slot_ids[None, :, None]) & member.T[:, None, :]
    slot_weight = jnp.sum(
        jnp.where(
            pick[:, :, None, :],
            table.reshape(row_count, sp_count, experts_dev).transpose(1, 2, 0)[:, None],
            0.0,
        ),
        axis=3,
    )
    weight_high = slot_weight.astype(low)
    weight_low = (slot_weight - weight_high.astype(jnp.float32)).astype(low)
    pick_matrix = pick.astype(low).reshape(sp_count * slots, row_count)
    outgoing = jnp.dot(pick_matrix, normed, preferred_element_type=jnp.float32).astype(low)
    extra = jnp.concatenate([weight_high, weight_low], axis=2)
    extra = jnp.pad(extra, ((0, 0), (0, 0), (0, 128 - extra.shape[2])))
    outgoing = jnp.concatenate([outgoing.reshape(sp_count, slots, model), extra], axis=2)
    arrived = swap_sp(outgoing, sp_count, 2)
    rows = sp_count * slots
    expert_part = experts_over_tp(
        arrived.reshape(rows, model + 128), gate_weight, up_weight, down_weight, tp_count, 3
    )
    expert_out = reduce_tp(expert_part, tp_count, 4).astype(low)
    returned = swap_sp(expert_out.reshape(sp_count, slots, model), sp_count, 5)
    expert_mix = jnp.dot(
        pick_matrix.T, returned.reshape(rows, model), preferred_element_type=jnp.float32
    )
    return (mixed_rows + expert_mix).astype(low)


def solution(mesh):
    return jax.shard_map(
        local,
        mesh=mesh,
        in_specs=(
            P(("sp", "tp"), None),
            P("sp", "tp", None),
            P("sp", "tp", None),
            P("sp", None),
            P("sp", None),
            P(),
            P(None, "tp", None),
            P(None, "tp", None),
            P("tp", None, None),
            P(),
            P("sp", None),
            P(("sp", "tp")),
            P(("sp", "tp"), None),
            P("sp", None, "tp"),
            P("sp", None, "tp"),
            P("sp", "tp", None),
        ),
        out_specs=P(("sp", "tp"), None),
        check_vma=False,
    )
```
